32 devices in a mesh: sp: 8 (over z, y), tp: 4 (over x, core).
Axes of the slice: x: 2, y: 2, z: 4, core: 2. Of those that a mesh axis runs over, the one named last changes fastest.
Arguments:
- tokens: bfloat16 [1536, 2048], P('sp', 'tp'), may hold values from -6 to 6
- norm_gain: float32 [2048], replicated, may hold values from 0.1 to 1.9
- query_weight: bfloat16 [2048, 512], P('sp', 'tp'), may hold values from -0.125 to 0.125
- key_weight: bfloat16 [2048, 512], P('sp', 'tp'), may hold values from -0.125 to 0.125
- value_weight: bfloat16 [2048, 512], P('sp', 'tp'), may hold values from -0.125 to 0.125
- decay_weight: bfloat16 [2048, 512], P('sp', 'tp'), may hold values from -0.09375 to 0.09375
- removal_weight: bfloat16 [2048, 512], P('sp', 'tp'), may hold values from -0.125 to 0.125
- gate_weight: bfloat16 [2048, 512], P('sp', 'tp'), may hold values from -0.125 to 0.125
- key_gain: float32 [512], P('tp'), may hold values from 0.1 to 1.9
- removal_gain: float32 [512], P('tp'), may hold values from 0.1 to 1.9
- removal_bias: float32 [512], P('tp'), may hold values from -9 to 1
- decay_bias: float32 [512], P('tp'), may hold values from -12.7 to -1.8
- decay_extra: float32 [1536, 512], P('sp', 'tp'), may hold values from 0 to 0.7
- scan_norm_gain: float32 [512], P('tp'), may hold values from 0.1 to 1.9
- conv_value_weight: bfloat16 [2048, 512], P('sp', 'tp'), may hold values from -0.125 to 0.125
- conv_gate_weight: bfloat16 [2048, 512], P('sp', 'tp'), may hold values from -0.125 to 0.125
- conv_kernel: float32 [31, 512], P(None, 'tp'), may hold values from -2 to 2
- conv_bias: float32 [512], P('tp'), may hold values from -2 to 3
- conv_norm_gain: float32 [512], P('tp'), may hold values from 0.1 to 1.9
- out_scan_weight: bfloat16 [512, 2048], P('tp', 'sp'), may hold values from -0.1875 to 0.1875
- out_conv_weight: bfloat16 [512, 2048], P('tp', 'sp'), may hold values from -0.1875 to 0.1875
Outputs:
- mixed: bfloat16 [1536, 2048], P('sp', 'tp')
The draws below stay inside these ranges and needn't reach their ends.
All inputs are finite; a program needn't handle non-finite values.
Results may differ from the reference program's by a relative error of at most 0.0073.
Values may be sent and summed in bfloat16 or wider, within the bound.
A program may use at most 64 MiB of HBM per device.

```python
import math
import jax
import jax.numpy as jnp
from jax import lax

MODEL = 2048
HEADS = 8
HEAD_SIZE = 64
CONV_K = 31
TOK_DEV = 192
WIDTH = 512
TOKENS = 1536


def head_ranks(key):
    return jax.random.permutation(jax.random.fold_in(key, 5), HEADS)


def slow_count():
    return HEADS // 2


def draw_decay_bias(key, part):
    ranks = head_ranks(key)
    jitter_key = jax.random.fold_in(key, 11)
    slow_heads = ranks < slow_count()
    jitter = jax.random.uniform(jitter_key, (WIDTH,), jnp.float32, -0.7, 0.7)
    centers = jnp.repeat(jnp.where(slow_heads, -12.0, -2.5), HEAD_SIZE)
    return (centers + jitter).astype(jnp.float32)


def draw_removal_bias(key, part):
    ranks = head_ranks(key)
    jitter_key = jax.random.fold_in(key, 13)
    lasting = max(1, HEADS // 4)
    keeping = ranks < lasting
    jitter = jax.random.uniform(jitter_key, (WIDTH,), jnp.float32, -1.0, 1.0)
    centers = jnp.repeat(jnp.where(keeping, -8.0, 0.0), HEAD_SIZE)
    return (centers + jitter).astype(jnp.float32)


def draw_decay_extra(key, part):
    keys = jax.random.split(jax.random.fold_in(key, 23), 3)
    spans = TOKENS // TOK_DEV
    levels = jnp.exp(jax.random.uniform(keys[0], (spans, HEADS), jnp.float32, math.log(3e-06), math.log(2.4e-05)))
    baseline = jnp.repeat(jnp.repeat(levels, TOK_DEV, axis=0), HEAD_SIZE, axis=1)
    places = jax.random.randint(keys[1], (3,), 0, TOKENS)
    hits = jnp.any(jnp.arange(TOKENS)[:, None] == places[None, :], axis=1)
    lowest = 0.22
    sizes = jnp.repeat(jax.random.uniform(keys[2], (TOKENS, HEADS), jnp.float32, lowest, 0.69), HEAD_SIZE, axis=1)
    return (baseline + jnp.where(hits[:, None], sizes, 0.0)).astype(jnp.float32)


def draw_conv_kernel(key, part):
    keys = jax.random.split(jax.random.fold_in(key, 37), 2)
    reach = 0.8
    rising = jnp.exp(jnp.linspace(-reach, reach, WIDTH))
    jitter = jnp.exp(jax.random.uniform(keys[0], (WIDTH,), jnp.float32, -0.3, 0.3))
    taps = jax.random.normal(keys[1], (CONV_K, WIDTH), jnp.float32) * CONV_K ** (-0.5)
    return jnp.clip(taps * rising * jitter, -2.0, 2.0).astype(jnp.float32)


def draw_conv_bias(key, part):
    jitter = jax.random.uniform(jax.random.fold_in(key, 41), (WIDTH,), jnp.float32, -0.4, 0.4)
    rising = jnp.linspace(-1.5, 1.5, WIDTH)
    return jnp.clip(rising + jitter, -2.0, 3.0).astype(jnp.float32)


def steps_of(rng, dims, cuts, low, high):
    loudness = 1.0
    for position, blocks in cuts:
        steps = jax.random.uniform(jax.random.fold_in(jax.random.fold_in(rng, 6), position), (blocks,), jnp.float32, low / len(cuts), high / len(cuts))
        loudness = loudness * jnp.repeat(jnp.exp(steps), dims[position] // blocks).reshape((-1,) + (1,) * (len(dims) - 1 - position))
    return loudness


def noise(key, shape, width, most, cuts=(), kind=jnp.bfloat16):
    result = jax.random.normal(key, shape, jnp.float32) * width
    if len(cuts) > 0:
        result = steps_of(key, shape, cuts, -0.22, 0.18) * result
    return jnp.clip(result, min=-most, max=most).astype(kind)


def setup_inputs(seed: int = 0) -> dict:
    key_of = jax.random.split(jax.random.key(seed), 22)
    return {
        "tokens": noise(key_of[0], (TOKENS, MODEL), 1.0, 6.0, ((0, 8), (1, 4))),
        "norm_gain": jnp.clip(1.0 + 0.18 * jax.random.normal(key_of[1], (MODEL,), jnp.float32), 0.1, 1.9),
        "query_weight": noise(key_of[2], (MODEL, WIDTH), MODEL ** -0.5, 0.125, ((0, 8), (1, 4))),
        "key_weight": noise(key_of[3], (MODEL, WIDTH), MODEL ** -0.5, 0.125, ((0, 8), (1, 4))),
        "value_weight": noise(key_of[4], (MODEL, WIDTH), MODEL ** -0.5, 0.125, ((0, 8), (1, 4))),
        "decay_weight": noise(key_of[5], (MODEL, WIDTH), (2 * MODEL) ** -0.5, 0.09375, ((0, 8), (1, 4))),
        "removal_weight": noise(key_of[6], (MODEL, WIDTH), MODEL ** -0.5, 0.125, ((0, 8), (1, 4))),
        "gate_weight": noise(key_of[7], (MODEL, WIDTH), MODEL ** -0.5, 0.125, ((0, 8), (1, 4))),
        "key_gain": jnp.clip(1.0 + 0.18 * jax.random.normal(key_of[8], (WIDTH,), jnp.float32), 0.1, 1.9),
        "removal_gain": jnp.clip(1.0 + 0.18 * jax.random.normal(key_of[9], (WIDTH,), jnp.float32), 0.1, 1.9),
        "removal_bias": draw_removal_bias(jax.random.fold_in(key_of[21], 71), 0),
        "decay_bias": draw_decay_bias(jax.random.fold_in(key_of[21], 71), 0),
        "decay_extra": draw_decay_extra(jax.random.fold_in(key_of[21], 71), 0),
        "scan_norm_gain": jnp.clip(1.0 + 0.18 * jax.random.normal(key_of[13], (WIDTH,), jnp.float32), 0.1, 1.9),
        "conv_value_weight": noise(key_of[14], (MODEL, WIDTH), MODEL ** -0.5, 0.125, ((0, 8), (1, 4))),
        "conv_gate_weight": noise(key_of[15], (MODEL, WIDTH), MODEL ** -0.5, 0.125, ((0, 8), (1, 4))),
        "conv_kernel": draw_conv_kernel(jax.random.fold_in(key_of[21], 71), 0),
        "conv_bias": draw_conv_bias(jax.random.fold_in(key_of[21], 71), 0),
        "conv_norm_gain": jnp.clip(1.0 + 0.18 * jax.random.normal(key_of[18], (WIDTH,), jnp.float32), 0.1, 1.9),
        "out_scan_weight": noise(key_of[19], (WIDTH, MODEL), (2 * WIDTH) ** -0.5, 0.1875, ((0, 4), (1, 8))),
        "out_conv_weight": noise(key_of[20], (WIDTH, MODEL), (2 * WIDTH) ** -0.5, 0.1875, ((0, 4), (1, 8))),
    }


def reference(tokens, norm_gain, query_weight, key_weight, value_weight, decay_weight, removal_weight, gate_weight, key_gain, removal_gain, removal_bias, decay_bias, decay_extra, scan_norm_gain, conv_value_weight, conv_gate_weight, conv_kernel, conv_bias, conv_norm_gain, out_scan_weight, out_conv_weight):
    exact_setting = lax.Precision.HIGHEST
    floats = tokens.astype(jnp.float32)
    normed = (floats * lax.rsqrt(lax.optimization_barrier(jnp.mean(floats * floats, axis=-1, keepdims=True)) + 1e-06) * norm_gain).astype(jnp.bfloat16)
    matrices = (query_weight, key_weight, value_weight, decay_weight, removal_weight, gate_weight, conv_value_weight, conv_gate_weight)
    stored = tuple((jnp.dot(normed, matrix, preferred_element_type=jnp.float32).astype(jnp.bfloat16) for matrix in matrices))
    stored = lax.optimization_barrier(stored)
    recept, key_rows, value_rows, decay_pre, removal_pre, gate_pre, conv_value, conv_gate = [item.astype(jnp.float32) for item in stored]
    decay_rate = jnp.exp(-jax.nn.softplus(-(decay_bias + decay_pre)) - 0.5) + decay_extra
    decay_factor = jnp.exp(-decay_rate)
    removal = jax.nn.sigmoid(removal_bias + removal_pre)

    def split_heads(table):
        return table.reshape(TOKENS, HEADS, HEAD_SIZE)
    scaled = split_heads(key_rows * key_gain)
    unit_keys = scaled * lax.rsqrt(lax.optimization_barrier(jnp.sum(scaled * scaled, axis=-1, keepdims=True)) + 1e-06)
    written = key_rows * (1.0 + (removal - 1.0) * removal_gain)

    def advance(memory, inputs):
        recept_t, decay_t, written_t, value_t, unit_t, removal_t = inputs
        removed_value = jnp.einsum('hvk,hk->hv', memory, -unit_t, precision=exact_setting)
        memory = memory * decay_t[:, None, :] + removed_value[:, :, None] * (unit_t * removal_t)[:, None, :] + value_t[:, :, None] * written_t[:, None, :]
        return (memory, jnp.einsum('hvk,hk->hv', memory, recept_t, precision=exact_setting))
    initial = jnp.zeros((HEADS, HEAD_SIZE, HEAD_SIZE), jnp.float32)
    _, reads = lax.scan(advance, initial, (split_heads(recept), split_heads(decay_factor), split_heads(written), split_heads(value_rows), unit_keys, split_heads(removal)))
    center = lax.optimization_barrier(jnp.mean(reads, axis=-1, keepdims=True))
    spread = lax.optimization_barrier(jnp.mean((reads - center) ** 2, axis=-1, keepdims=True))
    normalized = ((reads - center) * lax.rsqrt(spread + 0.00064)).reshape(TOKENS, WIDTH)
    scan_out = (normalized * scan_norm_gain * jax.nn.sigmoid(gate_pre)).astype(jnp.bfloat16)
    conv_input = (conv_value * jax.nn.sigmoid(conv_gate)).astype(jnp.bfloat16)
    padded = jnp.concatenate([jnp.zeros((CONV_K - 1, WIDTH), jnp.float32), conv_input.astype(jnp.float32)], axis=0)
    filtered = conv_bias + conv_kernel[0] * padded[0:TOKENS]
    for index in range(1, CONV_K):
        filtered = filtered + conv_kernel[index] * padded[index:index + TOKENS]
    channel_mean = lax.optimization_barrier(jnp.mean(filtered, axis=-1, keepdims=True))
    channel_var = lax.optimization_barrier(jnp.mean((filtered - channel_mean) ** 2, axis=-1, keepdims=True))
    conv_out = jax.nn.silu((filtered - channel_mean) * lax.rsqrt(channel_var + 1e-05) * conv_norm_gain).astype(jnp.bfloat16)
    total = jnp.dot(scan_out, out_scan_weight, preferred_element_type=jnp.float32) + jnp.dot(conv_out, out_conv_weight, preferred_element_type=jnp.float32)
    return total.astype(jnp.bfloat16)
```

```python
import functools

import jax
import jax.numpy as jnp
from jax import lax
from jax.experimental import pallas as pl
from jax.experimental.pallas import tpu as pltpu
from jax.sharding import PartitionSpec as P

HEAD_SIZE = 64
CONV_K = 31
HALO = 32
BLOCK = 32
SEGMENT = 96
MESH = pl.DeviceIdType.MESH

exact_setting = lax.Precision.HIGHEST


def remote(src, dst, send, recv, sp, tp):
    return pltpu.make_async_remote_copy(
        src_ref=src, dst_ref=dst, send_sem=send, recv_sem=recv,
        device_id={"sp": sp, "tp": tp}, device_id_type=MESH,
    )


def project_kernel(
    nsp, ntp, tokens, gain, weights, extra, outw,
    proj, extra_all, outw_all,
    tok, normed, full,
    send_y, recv_w, send_up, send_dn, send_tok, recv_tok, send_halo, recv_halo,
    send_out, recv_out, send_fwd, send_ex, recv_ex, local,
):
    s, t = lax.axis_index("sp"), lax.axis_index("tp")
    p, y = s // 2, s % 2
    np_ = nsp // 2
    mate = 2 * p + 1 - y
    rows = tokens.shape[0]
    depth = weights.shape[1]
    group = nsp // ntp
    half = group // 2

    def slot(b):
        return full.at[pl.ds(pl.multiple_of(b * depth, depth), depth), :]

    def place(yy, q):
        return tok.at[q, pl.ds(pl.multiple_of(HALO + yy * rows, 16), rows), :]

    def weight_copy(b, yy, sems, to):
        i = 2 * b + yy
        return remote(slot(i), slot(i), sems.at[i], recv_w.at[i], 2 * to + y, t)

    own = pltpu.make_async_copy(weights.at[y], slot(s), local.at[0])
    own.start()
    swap = remote(weights.at[1 - y], slot(s), send_y.at[0], recv_w.at[s], mate, t)
    swap.start()

    def send_own(sems, to):
        return remote(weights.at[y], slot(s), sems.at[s], recv_w.at[s], 2 * to + y, t)

    @pl.when(p + 1 < np_)
    def _():
        send_own(send_up, p + 1).start()

    @pl.when(p > 0)
    def _():
        send_own(send_dn, p - 1).start()

    mine = pltpu.make_async_copy(tokens, place(y, t), local.at[1])
    mine.start()
    group_size = 2 * ntp
    me = y * ntp + t

    def tok_send(d):
        g = lax.rem(me + d, group_size)
        return remote(tokens, place(y, t), send_tok.at[d], recv_tok.at[me], 2 * p + g // ntp, g % ntp)

    def halo_send(g):
        return remote(
            tokens.at[pl.ds(rows - HALO, HALO), :], tok.at[t, pl.ds(0, HALO), :],
            send_halo.at[g], recv_halo.at[t], 2 * (p + 1) + g // ntp, g % ntp,
        )

    for d in range(1, group_size):
        tok_send(d).start()
    sends_halo = jnp.logical_and(y == 1, p + 1 < np_)

    @pl.when(sends_halo)
    def _():
        for g in range(group_size):
            halo_send(g).start()

    ex_own = pltpu.make_async_copy(extra.at[y], extra_all.at[y], local.at[2])
    ex_own.start()
    ex = remote(extra.at[1 - y], extra_all.at[y], send_ex.at[0], recv_ex.at[0], mate, t)
    ex.start()

    j, q_to = s % group, s // group
    y_to = j // half

    def out_send(k):
        return remote(
            outw, outw_all.at[j, t], send_out.at[k], recv_out.at[j * ntp + t], 2 * k + y_to, q_to
        )

    def is_self(k):
        return jnp.logical_and(2 * k + y_to == s, q_to == t)

    def out_local():
        return pltpu.make_async_copy(outw, outw_all.at[j, t], recv_out.at[j * ntp + t])

    def start_out(k, c):
        @pl.when(is_self(k))
        def _():
            out_local().start()

        @pl.when(jnp.logical_not(is_self(k)))
        def _():
            out_send(k).start()

        return c

    own.wait()
    remote(slot(mate), slot(mate), send_y.at[0], recv_w.at[mate], mate, t).wait_recv()

    @pl.when(p + 1 < np_)
    def _():
        weight_copy(p, 1 - y, send_up, p + 1).start()

    @pl.when(p > 0)
    def _():
        weight_copy(p, 1 - y, send_dn, p - 1).start()

    lax.fori_loop(0, np_, start_out, 0)

    def line(k, c):
        for e in range(2):
            yy = lax.rem(y + e, 2)
            low, high = p - k, p + k

            @pl.when(low >= 0)
            def _():
                weight_copy(low, yy, send_up, p).wait_recv()

                @pl.when(p + 1 < np_)
                def _():
                    weight_copy(low, yy, send_up, p + 1).start()

            @pl.when(high < np_)
            def _():
                weight_copy(high, yy, send_dn, p).wait_recv()

                @pl.when(p > 0)
                def _():
                    weight_copy(high, yy, send_dn, p - 1).start()

        return c

    lax.fori_loop(1, 2, line, 0)

    mine.wait()
    for d in range(1, group_size):
        g = lax.rem(me + d, group_size)
        view = place(g // ntp, g % ntp)
        remote(view, view, send_tok.at[0], recv_tok.at[g], mate, t).wait_recv()

    @pl.when(p > 0)
    def _():
        for q in range(ntp):
            view = tok.at[q, pl.ds(0, HALO), :]
            remote(view, view, send_tok.at[0], recv_halo.at[q], mate, t).wait_recv()

    @pl.when(p == 0)
    def _():
        tok[:, 0:HALO, :] = jnp.zeros((ntp, HALO, tok.shape[2]), tok.dtype)

    width = tok.shape[2]
    total_rows = tok.shape[1]
    tile = HALO

    def norm_tile(i, c):
        at = pl.ds(pl.multiple_of(i * tile, tile), tile)
        squares = jnp.zeros((tile, 1), jnp.float32)
        for q in range(ntp):
            x = tok[q, at, :].astype(jnp.float32)
            squares = squares + jnp.sum(x * x, axis=-1, keepdims=True)
        scale = lax.rsqrt(squares / (ntp * width) + 1e-06)
        for q in range(ntp):
            x = tok[q, at, :].astype(jnp.float32)
            g = gain[:, q * width : (q + 1) * width]
            normed[at, q * width : (q + 1) * width] = (x * scale * g).astype(jnp.bfloat16)
        return c

    lax.fori_loop(0, total_rows // tile, norm_tile, 0)
    lax.fori_loop(2, np_, line, 0)

    def out_view(i):
        return outw_all.at[i // ntp, i % ntp]

    def forward(i):
        return remote(out_view(i), out_view(i), send_fwd.at[i], recv_out.at[i], mate, t)

    base = y * half * ntp
    other = (1 - y) * half * ntp

    def start_forward(i, c):
        forward(base + i).wait_recv()
        forward(base + i).start()
        return c

    lax.fori_loop(0, half * ntp, start_forward, 0)

    columns = full.shape[1]
    for n in range(0, columns, 256):
        proj[:, n : n + 256] = jnp.dot(
            normed[...], full[:, n : n + 256], preferred_element_type=jnp.float32
        ).astype(jnp.bfloat16)

    def end_forward(i, c):
        forward(other + i).wait_recv()
        forward(base + i).wait_send()
        return c

    lax.fori_loop(0, half * ntp, end_forward, 0)
    swap.wait_send()
    ex_own.wait()
    ex.wait()
    for d in range(1, group_size):
        tok_send(d).wait_send()

    @pl.when(sends_halo)
    def _():
        for g in range(group_size):
            halo_send(g).wait_send()

    def end_out(k, c):
        @pl.when(jnp.logical_not(is_self(k)))
        def _():
            out_send(k).wait_send()

        for yy in range(2):

            @pl.when(jnp.logical_and(k <= p, p + 1 < np_))
            def _():
                weight_copy(k, yy, send_up, p).wait_send()

            @pl.when(jnp.logical_and(k >= p, p > 0))
            def _():
                weight_copy(k, yy, send_dn, p).wait_send()

        return c

    lax.fori_loop(0, np_, end_out, 0)


def state_kernel(nsp, ntp, state, stats, states, stats_all, send_st, recv_st, send_g, recv_g, local):
    s, t = lax.axis_index("sp"), lax.axis_index("tp")
    p, y = s // 2, s % 2
    np_ = nsp // 2
    group_size = 2 * ntp
    me = y * ntp + t

    def st(k):
        return remote(state, states.at[p], send_st.at[k], recv_st.at[p], 2 * k + y, t)

    def st_in(k):
        return remote(states.at[k], states.at[k], send_st.at[k], recv_st.at[k], 2 * k + y, t)

    def start(k, c):
        st(k).start()
        return c

    lax.fori_loop(p + 1, np_, start, 0)
    copy = pltpu.make_async_copy(stats, stats_all.at[me], local.at[0])
    copy.start()

    def send(d):
        g = lax.rem(me + d, group_size)
        return remote(stats, stats_all.at[me], send_g.at[d], recv_g.at[me], 2 * p + g // ntp, g % ntp)

    for d in range(1, group_size):
        send(d).start()
    for d in range(1, group_size):
        g = lax.rem(me + d, group_size)
        remote(stats_all.at[g], stats_all.at[g], send_g.at[d], recv_g.at[g], s, t).wait_recv()
        send(d).wait_send()
    copy.wait()

    def end_in(k, c):
        st_in(k).wait_recv()
        return c

    lax.fori_loop(0, p, end_in, 0)

    def end_out(k, c):
        st(k).wait_send()
        return c

    lax.fori_loop(p + 1, np_, end_out, 0)


def feature_kernel(ntp, features, gathered, send_g, recv_g, local):
    s, t = lax.axis_index("sp"), lax.axis_index("tp")
    p, y = s // 2, s % 2
    group_size = 2 * ntp
    me = 2 * t + y
    wide = features.shape[2]

    def columns(g):
        return gathered.at[:, pl.ds(pl.multiple_of(g * wide, 128), wide)]

    copy = pltpu.make_async_copy(features.at[y], columns(me), local.at[0])
    copy.start()

    def send(d):
        g = lax.rem(me + d, group_size)
        return remote(features.at[g % 2], columns(me), send_g.at[d], recv_g.at[me], 2 * p + g % 2, g // 2)

    for d in range(1, group_size):
        send(d).start()
    for d in range(1, group_size):
        g = lax.rem(me + d, group_size)
        remote(columns(g), columns(g), send_g.at[d], recv_g.at[g], s, t).wait_recv()
        send(d).wait_send()
    copy.wait()


def call(kernel, outs, scratch, *operands):
    vmem = pl.BlockSpec(memory_space=pltpu.VMEM)
    return pl.pallas_call(
        kernel,
        out_shape=outs,
        in_specs=[vmem] * len(operands),
        out_specs=jax.tree.map(lambda _: vmem, outs),
        scratch_shapes=scratch,
        compiler_params=pltpu.CompilerParams(
            has_side_effects=True, vmem_limit_bytes=40 * 1024 * 1024
        ),
    )(*operands)


def combine_states(earlier, later):
    first = jnp.einsum("hij,hjk->hik", later[0], earlier[0], precision=exact_setting)
    second = jnp.einsum("hij,hjk->hik", later[0], earlier[1], precision=exact_setting) + later[1]
    return (first, second)


def block_product(left, right):
    return jnp.einsum("nhij,nhjk->nhik", left, right, precision=exact_setting)


def pairwise(left, right):
    return jnp.einsum("nhtk,nhik->nhti", left, right, precision=exact_setting)


def local_scan(recept, key_rows, values, decay_pre, removal_pre, key_gain, removal_gain, removal_bias, decay_bias, decay_extra):
    length = recept.shape[0]
    segments = length // SEGMENT
    steps = SEGMENT // BLOCK
    decay_rate = jnp.exp(-jax.nn.softplus(-(decay_bias + decay_pre)) - 0.5) + decay_extra
    removal = jax.nn.sigmoid(removal_bias + removal_pre)
    scaled = key_rows * key_gain
    unit_keys = scaled * lax.rsqrt(jnp.sum(scaled * scaled, axis=-1, keepdims=True) + 1e-06)
    written = key_rows * (1.0 + (removal - 1.0) * removal_gain)

    def blocked(table):
        return table.reshape(segments, steps, BLOCK, HEAD_SIZE).transpose(1, 0, 2, 3)

    recept_b, written_b, values_b = blocked(recept), blocked(written), blocked(values)
    rate_b, unit_b, removal_b = blocked(decay_rate), blocked(unit_keys), blocked(removal)
    position = jnp.arange(BLOCK)
    strict = (position[:, None] > position[None, :]).astype(jnp.float32)
    inclusive = (position[:, None] >= position[None, :]).astype(jnp.float32)
    falling = -jnp.einsum("ti,nhik->nhtk", inclusive, rate_b, precision=exact_setting)
    before = falling + rate_b
    middle = falling[:, :, BLOCK // 2 : BLOCK // 2 + 1]
    ending = falling[:, :, BLOCK - 1 :]
    alpha = -unit_b
    beta = unit_b * removal_b
    alpha_mid = alpha * jnp.exp(before - middle)
    recept_mid = recept_b * jnp.exp(falling - middle)
    lift = jnp.exp(middle - falling)
    beta_mid = beta * lift
    keys_mid = written_b * lift
    alpha_beta = pairwise(alpha_mid, beta_mid) * strict
    alpha_keys = pairwise(alpha_mid, keys_mid) * strict
    recept_beta = pairwise(recept_mid, beta_mid) * inclusive
    recept_keys = pairwise(recept_mid, keys_mid) * inclusive
    inverse = jnp.eye(BLOCK, dtype=jnp.float32) + alpha_beta
    power = alpha_beta
    for index in range(BLOCK.bit_length() - 2):
        power = block_product(power, power)
        inverse = inverse + block_product(inverse, power)
    widened = jnp.concatenate([values_b, jnp.zeros_like(values_b)], axis=-1)
    rhs_local = block_product(alpha_keys, widened)
    read_local = block_product(recept_keys, widened)
    start_alpha = alpha * jnp.exp(before)
    start_recept = recept_b * jnp.exp(falling)
    drop = jnp.exp(ending - falling)
    end_beta = beta * drop
    end_keys = written_b * drop
    end_decay = jnp.exp(ending)[:, :, 0, :]
    identity = jnp.broadcast_to(jnp.eye(HEAD_SIZE, dtype=jnp.float32), (segments, HEAD_SIZE, HEAD_SIZE))
    state = jnp.concatenate([jnp.zeros_like(identity), identity], axis=-1)
    reads = []
    for n in range(steps):
        rows = jnp.einsum("qfl,qlz->qfz", start_alpha[n], state, precision=exact_setting) + rhs_local[n]
        removed = jnp.einsum("hti,hiv->htv", inverse[n], rows, precision=exact_setting)
        reads.append(
            jnp.einsum("qfl,qlz->qfz", start_recept[n], state, precision=exact_setting)
            + jnp.einsum("hti,hiv->htv", recept_beta[n], removed, precision=exact_setting)
            + read_local[n]
        )
        state = (
            end_decay[n][:, :, None] * state
            + jnp.einsum("pzw,pzb->pwb", end_beta[n], removed, precision=exact_setting)
            + jnp.einsum("pzw,pzb->pwb", end_keys[n], widened[n], precision=exact_setting)
        )
    reads = jnp.stack(reads, axis=1).reshape(segments, SEGMENT, 2 * HEAD_SIZE)
    return reads, state


def matmul(left, right):
    return jnp.dot(left, right, precision=exact_setting)


def shards(
    tokens, norm_gain, query_weight, key_weight, value_weight, decay_weight, removal_weight, gate_weight,
    key_gain, removal_gain, removal_bias, decay_bias, decay_extra, scan_norm_gain,
    conv_value_weight, conv_gate_weight, conv_kernel, conv_bias, conv_norm_gain,
    out_scan_weight, out_conv_weight,
):
    nsp, ntp = lax.axis_size("sp"), lax.axis_size("tp")
    s = lax.axis_index("sp")
    p, y = s // 2, s % 2
    npair = nsp // 2
    group = nsp // ntp
    rows = tokens.shape[0]
    length = 2 * rows
    matrices = (
        query_weight, key_weight, value_weight, decay_weight,
        removal_weight, gate_weight, conv_value_weight, conv_gate_weight,
    )
    halves = jnp.stack(
        [
            jnp.concatenate([m[:, h * HEAD_SIZE : (h + 1) * HEAD_SIZE] for m in matrices], axis=1)
            for h in range(2)
        ]
    )
    extra = jnp.stack([decay_extra[:, :HEAD_SIZE], decay_extra[:, HEAD_SIZE:]])
    outw = jnp.concatenate(
        [w[h * HEAD_SIZE : (h + 1) * HEAD_SIZE] for h in range(2) for w in (out_scan_weight, out_conv_weight)],
        axis=0,
    )
    depth, columns = halves.shape[1:]
    model = depth * nsp
    dma = pltpu.SemaphoreType.DMA
    proj, extra_all, outw_all = call(
        functools.partial(project_kernel, nsp, ntp),
        (
            jax.ShapeDtypeStruct((length + HALO, columns), jnp.bfloat16),
            jax.ShapeDtypeStruct((2, rows, HEAD_SIZE), jnp.float32),
            jax.ShapeDtypeStruct((group, ntp) + outw.shape, jnp.bfloat16),
        ),
        [
            pltpu.VMEM((ntp, length + HALO, tokens.shape[1]), jnp.bfloat16),
            pltpu.VMEM((length + HALO, model), jnp.bfloat16),
            pltpu.VMEM((model, columns), jnp.bfloat16),
            dma((1,)), dma((nsp,)), dma((nsp,)), dma((nsp,)),
            dma((2 * ntp,)), dma((2 * ntp,)), dma((2 * ntp,)), dma((ntp,)),
            dma((npair,)), dma((group * ntp,)), dma((group * ntp,)), dma((1,)), dma((1,)), dma((3,)),
        ],
        tokens, norm_gain.reshape(1, model), halves, extra, outw,
    )

    def half_of(a):
        return lax.dynamic_slice_in_dim(a, y * HEAD_SIZE, HEAD_SIZE, a.ndim - 1)

    floats = proj.astype(jnp.float32)
    pieces = [floats[:, i * HEAD_SIZE : (i + 1) * HEAD_SIZE] for i in range(len(matrices))]
    recept, key_rows, values, decay_pre, removal_pre, gate_pre = [a[HALO:] for a in pieces[:6]]
    reads, segment_state = local_scan(
        recept, key_rows, values, decay_pre, removal_pre,
        half_of(key_gain), half_of(removal_gain), half_of(removal_bias), half_of(decay_bias),
        extra_all.reshape(length, HEAD_SIZE),
    )
    segments = segment_state.shape[0]
    prefix = []
    total = None
    for j in range(segments):
        prefix.append(total)
        local = segment_state[j]
        if total is None:
            total = local
        else:
            moved = matmul(local[:, HEAD_SIZE:], total)
            total = moved + jnp.concatenate([local[:, :HEAD_SIZE], jnp.zeros_like(local[:, :HEAD_SIZE])], axis=1)

    padded = (pieces[6] * jax.nn.sigmoid(pieces[7])).astype(jnp.bfloat16).astype(jnp.float32)
    taps = half_of(conv_kernel)
    first = HALO - (CONV_K - 1)
    filtered = half_of(conv_bias) + taps[0] * padded[first : first + length]
    for index in range(1, CONV_K):
        filtered = filtered + taps[index] * padded[first + index : first + index + length]
    stats = jnp.stack([jnp.sum(filtered, axis=-1), jnp.sum(filtered * filtered, axis=-1)])

    states, stats_all = call(
        functools.partial(state_kernel, nsp, ntp),
        (
            jax.ShapeDtypeStruct((npair,) + total.shape, jnp.float32),
            jax.ShapeDtypeStruct((2 * ntp,) + stats.shape, jnp.float32),
        ),
        [dma((npair,)), dma((npair,)), dma((2 * ntp,)), dma((2 * ntp,)), dma((1,))],
        total, stats,
    )

    def step(k, incoming):
        item = lax.dynamic_index_in_dim(states, k, 0, False)
        moved = matmul(item[:, HEAD_SIZE:], incoming) + item[:, :HEAD_SIZE]
        return jnp.where(k < p, moved, incoming)

    incoming = jnp.zeros((HEAD_SIZE, HEAD_SIZE), jnp.float32)
    for k in range(npair - 1) if npair <= 8 else ():
        incoming = step(k, incoming)
    if npair > 8:
        incoming = lax.fori_loop(0, npair - 1, step, incoming)
    starts = []
    for j in range(segments):
        if prefix[j] is None:
            starts.append(incoming)
        else:
            starts.append(matmul(prefix[j][:, HEAD_SIZE:], incoming) + prefix[j][:, :HEAD_SIZE])
    read = reads[..., :HEAD_SIZE] + jnp.einsum(
        "yem,ymb->yeb", reads[..., HEAD_SIZE:], jnp.stack(starts), precision=exact_setting
    )
    read = read.reshape(length, HEAD_SIZE)
    center = jnp.mean(read, axis=-1, keepdims=True)
    spread = jnp.mean((read - center) ** 2, axis=-1, keepdims=True)
    scan_out = (
        (read - center) * lax.rsqrt(spread + 0.00064) * half_of(scan_norm_gain) * jax.nn.sigmoid(gate_pre)
    ).astype(jnp.bfloat16)

    totals = jnp.sum(stats_all, axis=0)
    channels = 2 * ntp * HEAD_SIZE
    center = totals[0] / channels
    spread = totals[1] / channels - center * center
    scaled = (filtered - center[:, None]) * lax.rsqrt(spread[:, None] + 1e-05) * half_of(conv_norm_gain)
    conv_out = jax.nn.silu(scaled).astype(jnp.bfloat16)
    features = jnp.concatenate([scan_out, conv_out], axis=1).reshape(2, rows, 2 * HEAD_SIZE)
    gathered = call(
        functools.partial(feature_kernel, ntp),
        jax.ShapeDtypeStruct((rows, 4 * ntp * HEAD_SIZE), jnp.bfloat16),
        [dma((2 * ntp,)), dma((2 * ntp,)), dma((1,))],
        features,
    )
    regrouped = outw_all.transpose(1, 2, 0, 3).reshape(gathered.shape[1], -1)
    return jnp.dot(gathered, regrouped, preferred_element_type=jnp.float32).astype(jnp.bfloat16)


def solution(mesh):
    two = P("sp", "tp")
    one = P("tp")
    placed = (
        two, P(), two, two, two, two, two, two, one, one, one, one, two, one,
        two, two, P(None, "tp"), one, one, P("tp", "sp"), P("tp", "sp"),
    )
    return jax.shard_map(shards, mesh=mesh, in_specs=placed, out_specs=two, check_vma=False)
```

```python
import functools

import jax
import jax.numpy as jnp
from jax import lax
from jax.experimental import pallas as pl
from jax.experimental.pallas import tpu as pltpu
from jax.sharding import PartitionSpec as P

HEAD_SIZE = 64
CONV_K = 31
HALO = 32
BLOCK = 64
MESH = pl.DeviceIdType.MESH


def remote(src, dst, send, recv, sp, tp):
    return pltpu.make_async_remote_copy(
        src_ref=src, dst_ref=dst, send_sem=send, recv_sem=recv,
        device_id={"sp": sp, "tp": tp}, device_id_type=MESH,
    )


def project_kernel(
    nsp, ntp, tokens, gain, weights, extra,
    proj, extra_all,
    tok, normed, full,
    send_y, recv_w, send_up, send_dn, send_tok, recv_tok, send_halo, recv_halo,
    send_ex, recv_ex, local,
):
    s, t = lax.axis_index("sp"), lax.axis_index("tp")
    p, y = s // 2, s % 2
    np_ = nsp // 2
    mate = 2 * p + 1 - y
    rows = tokens.shape[0]
    depth = weights.shape[1]

    def slot(b):
        return full.at[pl.ds(pl.multiple_of(b * depth, depth), depth), :]

    def place(yy, q):
        return tok.at[q, pl.ds(pl.multiple_of(HALO + yy * rows, 16), rows), :]

    def weight_copy(b, yy, sems, to):
        i = 2 * b + yy
        return remote(slot(i), slot(i), sems.at[i], recv_w.at[i], 2 * to + y, t)

    own = pltpu.make_async_copy(weights.at[y], slot(s), local.at[0])
    own.start()
    swap = remote(weights.at[1 - y], slot(s), send_y.at[0], recv_w.at[s], mate, t)
    swap.start()

    def send_own(sems, to):
        return remote(weights.at[y], slot(s), sems.at[s], recv_w.at[s], 2 * to + y, t)

    @pl.when(p + 1 < np_)
    def _():
        send_own(send_up, p + 1).start()

    @pl.when(p > 0)
    def _():
        send_own(send_dn, p - 1).start()

    mine = pltpu.make_async_copy(tokens, place(y, t), local.at[1])
    mine.start()
    group_size = 2 * ntp
    me = y * ntp + t

    def tok_send(d):
        g = lax.rem(me + d, group_size)
        return remote(tokens, place(y, t), send_tok.at[d], recv_tok.at[me], 2 * p + g // ntp, g % ntp)

    def halo_send(g):
        return remote(
            tokens.at[pl.ds(rows - HALO, HALO), :], tok.at[t, pl.ds(0, HALO), :],
            send_halo.at[g], recv_halo.at[t], 2 * (p + 1) + g // ntp, g % ntp,
        )

    for d in range(1, group_size):
        tok_send(d).start()
    sends_halo = jnp.logical_and(y == 1, p + 1 < np_)

    @pl.when(sends_halo)
    def _():
        for g in range(group_size):
            halo_send(g).start()

    ex_own = pltpu.make_async_copy(extra.at[y], extra_all.at[y], local.at[2])
    ex_own.start()
    ex = remote(extra.at[1 - y], extra_all.at[y], send_ex.at[0], recv_ex.at[0], mate, t)
    ex.start()

    own.wait()
    remote(slot(mate), slot(mate), send_y.at[0], recv_w.at[mate], mate, t).wait_recv()

    @pl.when(p + 1 < np_)
    def _():
        weight_copy(p, 1 - y, send_up, p + 1).start()

    @pl.when(p > 0)
    def _():
        weight_copy(p, 1 - y, send_dn, p - 1).start()

    def line(k, c):
        for e in range(2):
            yy = lax.rem(y + e, 2)
            low, high = p - k, p + k

            @pl.when(low >= 0)
            def _():
                weight_copy(low, yy, send_up, p).wait_recv()

                @pl.when(p + 1 < np_)
                def _():
                    weight_copy(low, yy, send_up, p + 1).start()

            @pl.when(high < np_)
            def _():
                weight_copy(high, yy, send_dn, p).wait_recv()

                @pl.when(p > 0)
                def _():
                    weight_copy(high, yy, send_dn, p - 1).start()

        return c

    lax.fori_loop(1, 2, line, 0)

    mine.wait()
    for d in range(1, group_size):
        g = lax.rem(me + d, group_size)
        view = place(g // ntp, g % ntp)
        remote(view, view, send_tok.at[0], recv_tok.at[g], mate, t).wait_recv()

    @pl.when(p > 0)
    def _():
        for q in range(ntp):
            view = tok.at[q, pl.ds(0, HALO), :]
            remote(view, view, send_tok.at[0], recv_halo.at[q], mate, t).wait_recv()

    @pl.when(p == 0)
    def _():
        tok[:, 0:HALO, :] = jnp.zeros((ntp, HALO, tok.shape[2]), tok.dtype)

    width = tok.shape[2]
    total_rows = tok.shape[1]
    tile = HALO

    def norm_tile(i, c):
        at = pl.ds(pl.multiple_of(i * tile, tile), tile)
        squares = jnp.zeros((tile, 1), jnp.float32)
        for q in range(ntp):
            x = tok[q, at, :].astype(jnp.float32)
            squares = squares + jnp.sum(x * x, axis=-1, keepdims=True)
        scale = lax.rsqrt(squares / (ntp * width) + 1e-06)
        for q in range(ntp):
            x = tok[q, at, :].astype(jnp.float32)
            g = gain[:, q * width : (q + 1) * width]
            normed[at, q * width : (q + 1) * width] = (x * scale * g).astype(jnp.bfloat16)
        return c

    lax.fori_loop(0, total_rows // tile, norm_tile, 0)
    lax.fori_loop(2, np_, line, 0)

    columns = full.shape[1]
    for n in range(0, columns, 256):
        proj[:, n : n + 256] = jnp.dot(
            normed[...], full[:, n : n + 256], preferred_element_type=jnp.float32
        ).astype(jnp.bfloat16)

    swap.wait_send()
    ex_own.wait()
    ex.wait()
    for d in range(1, group_size):
        tok_send(d).wait_send()

    @pl.when(sends_halo)
    def _():
        for g in range(group_size):
            halo_send(g).wait_send()

    def end_out(k, c):
        for yy in range(2):

            @pl.when(jnp.logical_and(k <= p, p + 1 < np_))
            def _():
                weight_copy(k, yy, send_up, p).wait_send()

            @pl.when(jnp.logical_and(k >= p, p > 0))
            def _():
                weight_copy(k, yy, send_dn, p).wait_send()

        return c

    lax.fori_loop(0, np_, end_out, 0)


def dot(left, right, contract=(1, 0)):
    def one(a, b):
        return lax.dot_general(
            a, b, (((contract[0],), (contract[1],)), ((), ())), preferred_element_type=jnp.float32
        )

    left_high, right_high = left.astype(jnp.bfloat16), right.astype(jnp.bfloat16)
    left_low = (left - left_high.astype(jnp.float32)).astype(jnp.bfloat16)
    right_low = (right - right_high.astype(jnp.float32)).astype(jnp.bfloat16)
    return one(left_high, right_high) + (one(left_high, right_low) + one(left_low, right_high))


def sigmoid(x):
    return 1.0 / (1.0 + jnp.exp(-x))


def mixer_kernel(
    nsp, ntp, proj, extra, key_gain, removal_gain, removal_bias, decay_bias, scan_gain,
    conv_bias, conv_gain, taps, outw,
    out,
    outw_all, reads, total_ref, states, padded, filt, stats, stats_all, features, gathered, prefix, arriving,
    send_out, recv_out, send_fwd, send_st, recv_st, send_g, recv_g, send_f, recv_f, local,
):
    s, t = lax.axis_index("sp"), lax.axis_index("tp")
    p, y = s // 2, s % 2
    np_ = nsp // 2
    mate = 2 * p + 1 - y
    group = nsp // ntp
    half = group // 2
    group_size = 2 * ntp
    length = 2 * extra.shape[1]
    rows = extra.shape[1]
    size = HEAD_SIZE

    j, q_to = s % group, s // group
    y_to = j // half

    def out_send(k):
        return remote(
            outw, outw_all.at[j, t], send_out.at[k], recv_out.at[j * ntp + t], 2 * k + y_to, q_to
        )

    def is_self(k):
        return jnp.logical_and(2 * k + y_to == s, q_to == t)

    def start_out(k, c):
        @pl.when(is_self(k))
        def _():
            pltpu.make_async_copy(outw, outw_all.at[j, t], recv_out.at[j * ntp + t]).start()

        @pl.when(jnp.logical_not(is_self(k)))
        def _():
            out_send(k).start()

        return c

    lax.fori_loop(0, np_, start_out, 0)

    def mine(ref):
        whole = ref[...]
        return jnp.where(y == 0, whole[:, :size], whole[:, size:])

    k_gain, r_gain, r_bias, d_bias = mine(key_gain), mine(removal_gain), mine(removal_bias), mine(decay_bias)

    def column(i, start, count):
        pair = proj[start : start + count, (i // 2) * 2 * size : (i // 2 + 1) * 2 * size]
        return pair[:, (i % 2) * size : (i % 2 + 1) * size].astype(jnp.float32)

    side = 2 * BLOCK
    row = lax.broadcasted_iota(jnp.int32, (side, side), 0)
    col = lax.broadcasted_iota(jnp.int32, (side, side), 1)
    same = row // BLOCK == col // BLOCK
    strict = jnp.logical_and(same, row > col)
    inclusive = jnp.logical_and(same, row >= col)
    same16 = row // 16 == col // 16
    same32 = row // 32 == col // 32
    tri = jnp.where(inclusive, 1.0, 0.0)
    unit = jnp.where(row == col, 1.0, 0.0)
    eye = unit[:size, :size]
    maps = []
    for n in range(length // side):
        at = n * side
        recept, keys, values, decay_pre, removal_pre = [column(i, HALO + at, side) for i in range(5)]
        member, begin = divmod(at, rows)
        if begin + side <= rows:
            more = extra[member, begin : begin + side, :]
        else:
            more = jnp.concatenate([extra[member, begin:rows, :], extra[member + 1, 0 : begin + side - rows, :]], axis=0)
        rate = sigmoid(d_bias + decay_pre) * jnp.exp(jnp.float32(-0.5)) + more
        removal = sigmoid(r_bias + removal_pre)
        scaled = keys * k_gain
        unit_keys = scaled * lax.rsqrt(jnp.sum(scaled * scaled, axis=-1, keepdims=True) + 1e-06)
        written = keys * (1.0 + (removal - 1.0) * r_gain)
        falling = -dot(tri, rate)
        before = falling + rate

        def spread_row(offset):
            return jnp.concatenate(
                [
                    jnp.broadcast_to(falling[b * BLOCK + offset : b * BLOCK + offset + 1, :], (BLOCK, size))
                    for b in range(2)
                ],
                axis=0,
            )

        middle, ending = spread_row(BLOCK // 2), spread_row(BLOCK - 1)
        alpha = -unit_keys
        beta = unit_keys * removal
        lift = jnp.exp(middle - falling)
        left = jnp.concatenate([alpha * jnp.exp(before - middle), recept * jnp.exp(falling - middle)], axis=0)
        right = jnp.concatenate([beta * lift, written * lift], axis=0)
        prod = dot(left, right, (1, 1))
        alpha_beta = jnp.where(strict, prod[:side, :side], 0.0)
        alpha_keys = jnp.where(strict, prod[:side, side:], 0.0)
        recept_beta = jnp.where(inclusive, prod[side:, :side], 0.0)
        recept_keys = jnp.where(inclusive, prod[side:, side:], 0.0)
        power = jnp.where(same16, alpha_beta, 0.0)
        solve = unit + power
        for _ in range(3):
            power = dot(power, power)
            solve = solve + dot(solve, power)
        for edge in (
            jnp.where(jnp.logical_and(same32, jnp.logical_not(same16)), alpha_beta, 0.0),
            jnp.where(same32, 0.0, alpha_beta),
        ):
            solve = solve + dot(solve, dot(edge, solve))
        both = dot(jnp.concatenate([alpha_keys, recept_keys], axis=0), values)
        removed = dot(solve, jnp.concatenate([both[:side], alpha * jnp.exp(before)], axis=1))
        reads[at : at + side, :] = jnp.concatenate(
            [both[side:], recept * jnp.exp(falling)], axis=1
        ) + dot(recept_beta, removed)
        drop = jnp.exp(ending - falling)
        end_beta, end_keys = beta * drop, written * drop
        for b in range(2):
            part = slice(b * BLOCK, (b + 1) * BLOCK)
            last = falling[(b + 1) * BLOCK - 1 : (b + 1) * BLOCK, :]
            maps.append(
                jnp.concatenate([dot(end_keys[part].T, values[part]), eye * jnp.exp(last)], axis=1)
                + dot(end_beta[part].T, removed[part])
            )

    total = None
    for n, local_map in enumerate(maps):
        prefix[n] = jnp.concatenate([jnp.zeros((size, size), jnp.float32), eye], axis=1) if total is None else total
        if total is None:
            total = local_map
        else:
            total = dot(local_map[:, size:], total) + jnp.concatenate(
                [local_map[:, :size], jnp.zeros((size, size), jnp.float32)], axis=1
            )
    total_ref[...] = total

    padded[...] = (
        (column(6, 0, length + HALO) * sigmoid(column(7, 0, length + HALO))).astype(jnp.bfloat16).astype(jnp.float32)
    )
    tap = mine(taps)
    first = HALO - (CONV_K - 1)
    bias = mine(conv_bias)
    ones = jnp.ones((8, size), jnp.float32)
    for n in range(length // side):
        at = n * side
        filtered = bias + tap[0:1] * padded[first + at : first + at + side, :]
        for i in range(1, CONV_K):
            filtered = filtered + tap[i : i + 1] * padded[first + i + at : first + i + at + side, :]
        filt[at : at + side, :] = filtered
        stats[0:8, at : at + side] = dot(ones, filtered, (1, 1))
        stats[8:16, at : at + side] = dot(ones, filtered * filtered, (1, 1))

    def st(k):
        return remote(total_ref, states.at[p], send_st.at[k], recv_st.at[p], 2 * k + y, t)

    def start_state(k, c):
        st(k).start()
        return c

    lax.fori_loop(p + 1, np_, start_state, 0)
    me = 2 * t + y

    def send_stats(d):
        g = lax.rem(me + d, group_size)
        return remote(stats, stats_all.at[me], send_g.at[d], recv_g.at[me], 2 * p + g % 2, g // 2)

    for d in range(1, group_size):
        send_stats(d).start()

    def out_view(i):
        return outw_all.at[i // ntp, i % ntp]

    def forward(i):
        return remote(out_view(i), out_view(i), send_fwd.at[i], recv_out.at[i], mate, t)

    base = y * half * ntp
    other = (1 - y) * half * ntp

    def start_forward(i, c):
        forward(base + i).wait_recv()
        forward(base + i).start()
        return c

    lax.fori_loop(0, half * ntp, start_forward, 0)

    def arrived(k, c):
        remote(states.at[k], states.at[k], send_st.at[k], recv_st.at[k], 2 * k + y, t).wait_recv()
        return c

    lax.fori_loop(0, p, arrived, 0)
    still = jnp.concatenate([jnp.zeros((size, size), jnp.float32), eye], axis=1)
    incoming = jnp.zeros((size, size), jnp.float32)
    for k in range(np_ - 1):
        item = jnp.where(k < p, states[k], still)
        incoming = dot(item[:, size:], incoming) + item[:, :size]
    gain = mine(scan_gain)
    arriving[0] = incoming

    def finish(n, c):
        at = pl.ds(pl.multiple_of(n * BLOCK, BLOCK), BLOCK)
        begin = dot(prefix[n, :, size:], arriving[n // np_count]) + prefix[n, :, :size]
        block = reads[at, :]
        read = block[:, :size] + dot(block[:, size:], begin)
        center = jnp.mean(read, axis=-1, keepdims=True)
        spread = jnp.mean((read - center) ** 2, axis=-1, keepdims=True)
        gate_at = pl.ds(pl.multiple_of(HALO + n * BLOCK, HALO), BLOCK)
        gate = sigmoid(proj[gate_at, 4 * size : 6 * size].astype(jnp.float32)[:, size:])
        features[at, 0:size] = (
            (read - center) * lax.rsqrt(spread + 0.00064) * gain * gate
        ).astype(jnp.bfloat16)
        return c

    np_count = length // BLOCK
    lax.fori_loop(0, np_count, finish, 0)
    totals = stats[...]
    for d in range(1, group_size):
        g = lax.rem(me + d, group_size)
        remote(stats_all.at[g], stats_all.at[g], send_g.at[d], recv_g.at[g], s, t).wait_recv()
        totals = totals + stats_all[g]
    totals = totals / (group_size * size)
    center = totals[0:8]
    inverse = lax.rsqrt(totals[8:16] - center * center + 1e-05)
    center, inverse = center.T, inverse.T
    scaled = (filt[...] - center[:, 0:1]) * inverse[:, 0:1] * mine(conv_gain)
    features[:, size:] = (scaled * sigmoid(scaled)).astype(jnp.bfloat16)

    def end_forward(i, c):
        forward(other + i).wait_recv()
        forward(base + i).wait_send()
        return c

    wide = 2 * size

    def columns(g):
        return gathered.at[:, pl.ds(pl.multiple_of(g * wide, 128), wide)]

    def part_of(yy):
        return features.at[pl.ds(pl.multiple_of(yy * rows, 16), rows), :]

    def send(d):
        g = lax.rem(me + d, group_size)
        return remote(part_of(g % 2), columns(me), send_f.at[d], recv_f.at[me], 2 * p + g % 2, g // 2)

    for d in range(1, group_size):
        send(d).start()
    copy = pltpu.make_async_copy(part_of(y), columns(me), local.at[0])
    copy.start()

    lax.fori_loop(0, half * ntp, end_forward, 0)

    def end_out(k, c):
        @pl.when(jnp.logical_not(is_self(k)))
        def _():
            out_send(k).wait_send()

        return c

    lax.fori_loop(0, np_, end_out, 0)

    def end_state(k, c):
        st(k).wait_send()
        return c

    lax.fori_loop(p + 1, np_, end_state, 0)
    for d in range(1, group_size):
        send_stats(d).wait_send()
    for d in range(1, group_size):
        g = lax.rem(me + d, group_size)
        remote(columns(g), columns(g), send_f.at[d], recv_f.at[g], s, t).wait_recv()
        send(d).wait_send()
    copy.wait()
    strip = outw.shape[1]
    for i in range(group):
        weight = outw_all[i].reshape(gathered.shape[1], strip)
        out[:, i * strip : (i + 1) * strip] = jnp.dot(
            gathered[...], weight, preferred_element_type=jnp.float32
        ).astype(jnp.bfloat16)


def call(kernel, outs, scratch, *operands):
    vmem = pl.BlockSpec(memory_space=pltpu.VMEM)
    return pl.pallas_call(
        kernel,
        out_shape=outs,
        in_specs=[vmem] * len(operands),
        out_specs=jax.tree.map(lambda _: vmem, outs),
        scratch_shapes=scratch,
        compiler_params=pltpu.CompilerParams(
            has_side_effects=True, vmem_limit_bytes=40 * 1024 * 1024
        ),
    )(*operands)


def shards(
    tokens, norm_gain, query_weight, key_weight, value_weight, decay_weight, removal_weight, gate_weight,
    key_gain, removal_gain, removal_bias, decay_bias, decay_extra, scan_norm_gain,
    conv_value_weight, conv_gate_weight, conv_kernel, conv_bias, conv_norm_gain,
    out_scan_weight, out_conv_weight,
):
    nsp, ntp = lax.axis_size("sp"), lax.axis_size("tp")
    npair = nsp // 2
    group = nsp // ntp
    rows = tokens.shape[0]
    length = 2 * rows
    matrices = (
        query_weight, key_weight, value_weight, decay_weight,
        removal_weight, gate_weight, conv_value_weight, conv_gate_weight,
    )
    halves = jnp.stack(
        [
            jnp.concatenate([m[:, h * HEAD_SIZE : (h + 1) * HEAD_SIZE] for m in matrices], axis=1)
            for h in range(2)
        ]
    )
    extra = jnp.stack([decay_extra[:, :HEAD_SIZE], decay_extra[:, HEAD_SIZE:]])
    outw = jnp.concatenate(
        [w[h * HEAD_SIZE : (h + 1) * HEAD_SIZE] for h in range(2) for w in (out_scan_weight, out_conv_weight)],
        axis=0,
    )
    depth, columns = halves.shape[1:]
    model = depth * nsp
    dma = pltpu.SemaphoreType.DMA
    proj, extra_all = call(
        functools.partial(project_kernel, nsp, ntp),
        (
            jax.ShapeDtypeStruct((length + HALO, columns), jnp.bfloat16),
            jax.ShapeDtypeStruct((2, rows, HEAD_SIZE), jnp.float32),
        ),
        [
            pltpu.VMEM((ntp, length + HALO, tokens.shape[1]), jnp.bfloat16),
            pltpu.VMEM((length + HALO, model), jnp.bfloat16),
            pltpu.VMEM((model, columns), jnp.bfloat16),
            dma((1,)), dma((nsp,)), dma((nsp,)), dma((nsp,)),
            dma((2 * ntp,)), dma((2 * ntp,)), dma((2 * ntp,)), dma((ntp,)),
            dma((1,)), dma((1,)), dma((3,)),
        ],
        tokens, norm_gain.reshape(1, model), halves, extra,
    )
    bf, f32 = jnp.bfloat16, jnp.float32
    group_size = 2 * ntp
    return call(
        functools.partial(mixer_kernel, nsp, ntp),
        jax.ShapeDtypeStruct((rows, group * outw.shape[1]), bf),
        [
            pltpu.VMEM((group, ntp) + outw.shape, bf),
            pltpu.VMEM((length, 2 * HEAD_SIZE), f32),
            pltpu.VMEM((HEAD_SIZE, 2 * HEAD_SIZE), f32),
            pltpu.VMEM((npair, HEAD_SIZE, 2 * HEAD_SIZE), f32),
            pltpu.VMEM((length + HALO, HEAD_SIZE), f32),
            pltpu.VMEM((length, HEAD_SIZE), f32),
            pltpu.VMEM((16, length), f32),
            pltpu.VMEM((group_size, 16, length), f32),
            pltpu.VMEM((length, 2 * HEAD_SIZE), bf),
            pltpu.VMEM((rows, group_size * 2 * HEAD_SIZE), bf),
            pltpu.VMEM((length // BLOCK, HEAD_SIZE, 2 * HEAD_SIZE), f32),
            pltpu.VMEM((1, HEAD_SIZE, HEAD_SIZE), f32),
            dma((npair,)), dma((group * ntp,)), dma((group * ntp,)),
            dma((npair,)), dma((npair,)),
            dma((group_size,)), dma((group_size,)), dma((group_size,)), dma((group_size,)), dma((1,)),
        ],
        proj, extra_all,
        *(
            a.reshape(1, -1)
            for a in (key_gain, removal_gain, removal_bias, decay_bias, scan_norm_gain, conv_bias, conv_norm_gain)
        ),
        conv_kernel, outw,
    )


def solution(mesh):
    two = P("sp", "tp")
    one = P("tp")
    placed = (
        two, P(), two, two, two, two, two, two, one, one, one, one, two, one,
        two, two, P(None, "tp"), one, one, P("tp", "sp"), P("tp", "sp"),
    )
    return jax.shard_map(shards, mesh=mesh, in_specs=placed, out_specs=two, check_vma=False)
```
